512 devices in a mesh: fs: 128 (over z, x, core), tp: 4 (over y).
Axes of the slice: x: 4, y: 4, z: 16, core: 2. Of those that a mesh axis runs over, the one named last changes fastest.
Arguments:
- tokens: bfloat16 [768, 4096], P('tp'), may hold values from -6 to 6
- norm_gain: float32 [4096], P('fs'), may hold values from 0.1 to 1.9
- gate_trained: float32 [4096, 11264], P('fs', 'tp'), may hold values from -0.09375 to 0.09375
- up_trained: float32 [4096, 11264], P('fs', 'tp'), may hold values from -0.09375 to 0.09375
- down_trained: float32 [11264, 4096], P('fs', 'tp'), may hold values from -0.21875 to 0.21875
Outputs:
- gate_sampler: bfloat16 [4096, 11264], P(None, 'fs')
- up_sampler: bfloat16 [4096, 11264], P(None, 'fs')
- down_sampler: bfloat16 [11264, 4096], P('fs')
- mixed_out: bfloat16 [768, 4096], P('tp', 'fs')
The draws below stay inside these ranges and needn't reach their ends.
All inputs are finite; a program needn't handle non-finite values.
Results may differ from the reference program's by a relative error of at most 0.0082.
Values may be sent and summed in bfloat16 or wider, within the bound.
A program may use at most 64 MiB of HBM per device.

```python
import jax
import jax.numpy as jnp
from jax import lax

D = 4096
FF = 11264
TOKENS = 768


def spiked(entries, own_key, source, target, shards_of, factor):
    def block_of(axis_at):
        return (jnp.arange(entries.shape[axis_at]) // (entries.shape[axis_at] // shards_of)).reshape((-1,) + (1,) * (entries.ndim - 1 - axis_at))

    first = jax.random.permutation(own_key, shards_of)[block_of(target)]
    second = (block_of(target) + shards_of // 2) % shards_of
    return jnp.where((block_of(source) == first) | (block_of(source) == second), factor * entries, entries)


def shard_levels(rng, dims, shards, least, largest):
    loudness, own = 1.0, jax.random.fold_in(rng, 6)
    for dim, blocks in shards:
        steps = jnp.exp(jax.random.uniform(jax.random.fold_in(own, dim), (blocks,), jnp.float32, least / len(shards), largest / len(shards)))
        loudness = loudness * jnp.repeat(steps, dims[dim] // blocks).reshape([-1 if axis == dim else 1 for axis in range(len(dims))])
    return loudness


def gaussian(own_key, shape, scale, limit, cuts=(), kind=jnp.bfloat16):
    array = scale * jax.random.normal(own_key, shape, jnp.float32)
    if cuts:
        array = array * shard_levels(own_key, shape, cuts, -0.22, 0.18)
    return jnp.clip(array, -limit, limit).astype(kind)


def gaussian_with(rng, shape, scale, reach, split, heavy, held_as=jnp.bfloat16):
    values = scale * jax.random.normal(rng, shape, jnp.float32)
    if split:
        values = values * shard_levels(rng, shape, split, -0.22, 0.18)
    return jnp.clip(spiked(values, jax.random.fold_in(rng, 3), *heavy), -reach, reach).astype(held_as)


def setup_inputs(seed: int = 0) -> dict:
    key_list = jax.random.split(jax.random.key(seed), 6)
    tokens = gaussian(key_list[0], (TOKENS, D), 1.0, 6.0, ((0, 4),))
    norm_gain = jnp.clip(1.0 + 0.18 * jax.random.normal(key_list[1], (D,), jnp.float32), 0.1, 1.9)
    gate_trained = gaussian(key_list[2], (D, FF), D ** -0.5, 0.09375, ((0, 128), (1, 4)), jnp.float32)
    up_trained = gaussian(key_list[3], (D, FF), D ** -0.5, 0.09375, ((0, 128), (1, 4)), jnp.float32)
    down_trained = gaussian_with(key_list[4], (FF, D), FF ** -0.5, 0.21875, ((0, 128), (1, 4)), (0, 1, 128, 5.5), jnp.float32)
    return {"tokens": tokens, "norm_gain": norm_gain, "gate_trained": gate_trained, "up_trained": up_trained, "down_trained": down_trained}


def reference(tokens, norm_gain, gate_trained, up_trained, down_trained):
    gate_sampler = (norm_gain[:, None] * gate_trained).astype(jnp.bfloat16)
    up_sampler = (norm_gain[:, None] * up_trained).astype(jnp.bfloat16)
    down_sampler = down_trained.astype(jnp.bfloat16)
    as_float = tokens.astype(jnp.float32)
    normed = (as_float * jax.lax.rsqrt(lax.optimization_barrier(jnp.mean(as_float * as_float, axis=-1, keepdims=True)) + 1e-06)).astype(jnp.bfloat16)
    gate_act = jnp.dot(normed, gate_sampler, preferred_element_type=jnp.float32)
    up_act = jnp.dot(normed, up_sampler, preferred_element_type=jnp.float32)
    hidden = (jax.nn.silu(gate_act) * up_act).astype(jnp.bfloat16)
    mixed_out = jnp.dot(hidden, down_sampler, preferred_element_type=jnp.float32).astype(jnp.bfloat16)
    return (gate_sampler, up_sampler, down_sampler, mixed_out)
```

```python
import jax
import jax.numpy as jnp
from jax import lax
from jax.experimental import pallas as pl
from jax.experimental.pallas import tpu as pltpu
from jax.sharding import Mesh
from jax.sharding import PartitionSpec as P

MESH = pl.DeviceIdType.MESH
BF = jnp.bfloat16
F32 = jnp.float32

NZ, NX, NC, NY = 16, 4, 2, 4
D, OWN, TOK, TPAD = 4096, 88, 192, 256
GROUP = 704


def lane_blocks_swapped(tiles):
    lane = lax.broadcasted_iota(jnp.int32, tiles[0].shape, 1) // 32
    outs = []
    for k in range(4):
        acc = None
        for t in range(4):
            shift = (32 * (t - k)) % 128
            moved = tiles[t] if shift == 0 else pltpu.roll(tiles[t], shift, 1)
            acc = moved if acc is None else jnp.where(lane == t, moved, acc)
        outs.append(acc)
    return outs


def kernel(
    tok, gain, gate, up, down, g_out, u_out, d_out, m_out,
    tok_v, gain_v, gu_v, down_v, normed, s_buf, ra, sb, rb, w, dn, db, d2, h, sr, rr, m_v,
    in_sem, out_sem,
    a_send, a_recv, b_send, b_recv, c_send, c_recv, d_send, d_recv, e_send, e_recv, h_send, h_recv, r_send, r_recv,
):
    z, x, c, y = (lax.axis_index(n) for n in ("z", "x", "c", "y"))
    xc = x * 2 + c
    barrier = pltpu.get_barrier_semaphore()
    here = xc * 4 + y

    def greet_plane(n, _):
        other = lax.rem(here + n, 32)
        pl.semaphore_signal(
            barrier, inc=1, device_id=(z, other // 8, lax.rem(other // 4, 2), lax.rem(other, 4)), device_id_type=MESH
        )
        return 0

    def greet_line(n, _):
        pl.semaphore_signal(barrier, inc=1, device_id=(lax.rem(z + n, NZ), x, c, y), device_id_type=MESH)
        return 0

    lax.fori_loop(1, NZ, greet_line, 0)
    lax.fori_loop(1, 32, greet_plane, 0)

    loads = [
        pltpu.make_async_copy(gate, gu_v.at[0], in_sem.at[0]),
        pltpu.make_async_copy(up, gu_v.at[1], in_sem.at[1]),
        pltpu.make_async_copy(gain, gain_v, in_sem.at[2]),
        pltpu.make_async_copy(down, down_v, in_sem.at[3]),
        pltpu.make_async_copy(tok, tok_v, in_sem.at[4]),
    ]
    for cp in loads:
        cp.start()
    loads[2].wait()
    gains = jnp.concatenate([gain_v[...]] * 4, axis=1)
    for g in range(2):
        loads[g].wait()
        stacked = jnp.concatenate([gu_v[g, :, GROUP * q : GROUP * (q + 1)] for q in range(4)], axis=0)
        turned = (jnp.transpose(stacked) * gains).astype(BF)
        for k in range(8):
            s_buf[g, k] = turned[OWN * k : OWN * (k + 1)]
    loads[3].wait()
    down_bf = down_v[...].astype(BF)
    dn[:, pl.ds(pl.multiple_of(1024 * y, 1024), 1024)] = down_bf

    pl.semaphore_wait(barrier, 46)

    half = x // 2
    sub = lax.rem(x, 2) * 2 + c

    def a_copy(n):
        to_x, to_y = lax.rem(x + n // 4, NX), lax.rem(y + n, NY)
        return pltpu.make_async_remote_copy(
            src_ref=s_buf.at[lax.rem(to_y, 2), to_x * 2 + to_y // 2],
            dst_ref=ra.at[y, sub],
            send_sem=a_send.at[n],
            recv_sem=a_recv.at[y, sub],
            device_id=(z, to_x, half, to_y),
            device_id_type=MESH,
        )

    def a_start(n, _):
        a_copy(n).start()
        return 0

    @pl.when(half != c)
    def _():
        a_copy(0).start()

    @pl.when(half == c)
    def _():
        ra[y, sub] = s_buf[lax.rem(y, 2), x * 2 + y // 2]

    lax.fori_loop(1, 16, a_start, 0)

    def d_copy(n):
        at = dn.at[:, pl.ds(pl.multiple_of(1024 * y, 1024), 1024)]
        return pltpu.make_async_remote_copy(
            src_ref=at, dst_ref=at, send_sem=d_send.at[n], recv_sem=d_recv.at[y],
            device_id=(z, x, c, lax.rem(y + n, NY)), device_id_type=MESH,
        )

    for n in (1, 3, 2):
        d_copy(n).start()

    loads[4].wait()

    def norm_rows(n, _):
        rows = pl.ds(pl.multiple_of(n * 16, 16), 16)
        t = tok_v[rows, :].astype(F32)
        normed[rows, :] = (t * lax.rsqrt(jnp.mean(t * t, axis=-1, keepdims=True) + 1e-06)).astype(BF)
        return 0

    lax.fori_loop(0, TOK // 16, norm_rows, 0)
    normed[TOK:, :] = jnp.zeros((TPAD - TOK, D), BF)

    def a_arrived(ys, s):
        @pl.when(jnp.logical_or(half != c, jnp.logical_or(ys != y, s != sub)))
        def _():
            pltpu.make_async_remote_copy(
                src_ref=ra.at[ys, s], dst_ref=ra.at[ys, s], send_sem=a_send.at[0], recv_sem=a_recv.at[ys, s],
                device_id=(z, x, 1 - c, y), device_id_type=MESH,
            ).wait_recv()

    def regroup(ys, _):
        for s in range(4):
            a_arrived(ys, s)
        outs = lane_blocks_swapped([ra[ys, s].astype(F32) for s in range(4)])
        for q in range(4):
            sb[ys * 4 + q] = outs[q].astype(BF)
        return 0

    lax.fori_loop(0, NY, regroup, 0)

    def near_first(i):
        return jnp.where(lax.rem(i, 2) == 1, (i + 1) // 2, NZ - i // 2)

    def b_copy(i):
        to_z = lax.rem(z + near_first(i), NZ)
        return pltpu.make_async_remote_copy(
            src_ref=sb.at[to_z], dst_ref=rb.at[z], send_sem=b_send.at[i], recv_sem=b_recv.at[z],
            device_id=(to_z, x, c, y), device_id_type=MESH,
        )

    def b_start(i, _):
        b_copy(i).start()
        return 0

    lax.fori_loop(1, NZ, b_start, 0)
    rb[z] = sb[z]

    own_c, own_g = y // 2, lax.rem(y, 2)

    def w_lanes(zs):
        return pl.ds(pl.multiple_of(256 * zs + 128 * c, 128), 128)

    def c_copy(zs, n):
        return pltpu.make_async_remote_copy(
            src_ref=rb.at[zs], dst_ref=w.at[own_g, :, w_lanes(zs)], send_sem=c_send.at[n], recv_sem=c_recv.at[own_g, c],
            device_id=(z, x, own_c, lax.rem(y + n, NY)), device_id_type=MESH,
        )

    def c_spread(zs):
        for n in (1, 3, 2):
            c_copy(zs, n).start()

        @pl.when(own_c != c)
        def _():
            c_copy(zs, 0).start()

        @pl.when(own_c == c)
        def _():
            w[own_g, :, w_lanes(zs)] = rb[zs]

    c_spread(z)

    def c_step(i, _):
        zs = lax.rem(z + NZ - near_first(i), NZ)
        pltpu.make_async_remote_copy(
            src_ref=rb.at[zs], dst_ref=rb.at[zs], send_sem=b_send.at[0], recv_sem=b_recv.at[zs],
            device_id=(lax.rem(z + 1, NZ), x, c, y), device_id_type=MESH,
        ).wait_recv()
        c_spread(zs)
        return 0

    lax.fori_loop(1, 8, c_step, 0)

    for n in (1, 2, 3):
        ys = lax.rem(y + NY - n, NY)
        at = dn.at[:, pl.ds(pl.multiple_of(1024 * ys, 1024), 1024)]
        pltpu.make_async_remote_copy(
            src_ref=at, dst_ref=at, send_sem=d_send.at[0], recv_sem=d_recv.at[ys],
            device_id=(z, x, 1 - c, y), device_id_type=MESH,
        ).wait_recv()
    d_store = pltpu.make_async_copy(dn, d_out, out_sem.at[2])
    d_store.start()

    def by_column(n, _):
        ys, hi = n // 2, lax.rem(n, 2)
        tiles = [
            dn[:, pl.ds(pl.multiple_of(1024 * ys + 256 * q + 128 * hi, 128), 128)].astype(F32) for q in range(4)
        ]
        outs = lane_blocks_swapped(tiles)
        for k in range(4):
            db[hi * 4 + k, :, pl.ds(pl.multiple_of(128 * ys, 128), 128)] = outs[k].astype(BF)
        return 0

    lax.fori_loop(0, 8, by_column, 0)

    def e_copy(n):
        to = lax.rem(xc + n, 8)
        return pltpu.make_async_remote_copy(
            src_ref=db.at[to], dst_ref=d2.at[xc], send_sem=e_send.at[n], recv_sem=e_recv.at[xc],
            device_id=(z, to // 2, lax.rem(to, 2), y), device_id_type=MESH,
        )

    def e_start(n, _):
        e_copy(n).start()
        return 0

    lax.fori_loop(1, 8, e_start, 0)
    d2[xc] = db[xc]

    lax.fori_loop(8, NZ, c_step, 0)

    stores = [d_store]
    for g in range(2):
        for k in range(2):
            @pl.when(jnp.logical_or(y != 2 * c + g, c != k))
            def _():
                pltpu.make_async_remote_copy(
                    src_ref=rb, dst_ref=rb, send_sem=c_send.at[0], recv_sem=c_recv.at[g, k],
                    device_id=(z, x, 1 - c, y), device_id_type=MESH,
                ).wait_recv()
        stores.append(pltpu.make_async_copy(w.at[g], (g_out, u_out)[g], out_sem.at[g]))
        stores[-1].start()

    acts = [
        lax.dot_general(w[g], normed[...], (((1,), (1,)), ((), ())), preferred_element_type=F32) for g in range(2)
    ]
    h[xc] = (acts[0] / (1.0 + jnp.exp(-acts[0])) * acts[1]).astype(BF)

    def h_copy(n):
        to = lax.rem(xc + n, 8)
        return pltpu.make_async_remote_copy(
            src_ref=h.at[xc], dst_ref=h.at[xc], send_sem=h_send.at[n], recv_sem=h_recv.at[xc],
            device_id=(z, to // 2, lax.rem(to, 2), y), device_id_type=MESH,
        )

    def h_start(n, _):
        h_copy(n).start()
        return 0

    lax.fori_loop(1, 8, h_start, 0)

    def plane_arrived(n, _):
        fr = lax.rem(xc + 8 - n, 8)
        pltpu.make_async_remote_copy(
            src_ref=d2.at[fr], dst_ref=d2.at[fr], send_sem=e_send.at[0], recv_sem=e_recv.at[fr],
            device_id=(z, x, 1 - c, y), device_id_type=MESH,
        ).wait_recv()
        pltpu.make_async_remote_copy(
            src_ref=h.at[fr], dst_ref=h.at[fr], send_sem=h_send.at[0], recv_sem=h_recv.at[fr],
            device_id=(z, x, 1 - c, y), device_id_type=MESH,
        ).wait_recv()
        return 0

    lax.fori_loop(1, 8, plane_arrived, 0)
    part = lax.dot_general(
        d2[...].reshape(8 * OWN, 512), h[...].reshape(8 * OWN, TPAD), (((0,), (0,)), ((), ())),
        preferred_element_type=F32,
    )
    lane = lax.broadcasted_iota(jnp.int32, (16, 128), 1)
    for q in range(NZ):
        block = part[32 * q : 32 * (q + 1)]
        tail = block[:, 128:]
        sr[q, :32] = block[:, :128].astype(BF)
        sr[q, 32:] = jnp.where(lane < 64, tail[:16], pltpu.roll(tail[16:], 64, 1)).astype(BF)

    def r_copy(i):
        to_z = lax.rem(z + near_first(i), NZ)
        return pltpu.make_async_remote_copy(
            src_ref=sr.at[to_z], dst_ref=rr.at[z], send_sem=r_send.at[i], recv_sem=r_recv.at[z],
            device_id=(to_z, x, c, y), device_id_type=MESH,
        )

    def r_start(i, _):
        r_copy(NZ - i).start()
        return 0

    lax.fori_loop(1, NZ, r_start, 0)

    def r_arrived(i, total):
        zs = lax.rem(z + NZ - near_first(i), NZ)
        pltpu.make_async_remote_copy(
            src_ref=rr.at[zs], dst_ref=rr.at[zs], send_sem=r_send.at[0], recv_sem=r_recv.at[zs],
            device_id=(lax.rem(z + 1, NZ), x, c, y), device_id_type=MESH,
        ).wait_recv()
        return total + rr[zs].astype(F32)

    total = lax.fori_loop(1, NZ, r_arrived, sr[z].astype(F32))
    m_v[:, :128] = total[:32].astype(BF)
    m_v[:16, 128:] = total[32:, :64].astype(BF)
    m_v[16:, 128:] = pltpu.roll(total[32:], 64, 1)[:, :64].astype(BF)
    m_store = pltpu.make_async_copy(m_v, m_out, out_sem.at[3])
    m_store.start()
    stores.append(m_store)

    @pl.when(half != c)
    def _():
        a_copy(0).wait_send()

    def a_sent(n, _):
        a_copy(n).wait_send()
        return 0

    lax.fori_loop(1, 16, a_sent, 0)

    def line_sent(i, _):
        b_copy(i).wait_send()
        r_copy(i).wait_send()
        return 0

    lax.fori_loop(1, NZ, line_sent, 0)

    def plane_sent(n, _):
        e_copy(n).wait_send()
        h_copy(n).wait_send()
        return 0

    lax.fori_loop(1, 8, plane_sent, 0)

    def c_sent(n):
        pltpu.make_async_remote_copy(
            src_ref=rb, dst_ref=rb, send_sem=c_send.at[n], recv_sem=c_recv.at[0, 0],
            device_id=(z, x, 1 - c, y), device_id_type=MESH,
        ).wait_send()

    for n in (1, 2, 3):
        d_copy(n).wait_send()
        c_sent(n)

    @pl.when(own_c != c)
    def _():
        c_sent(0)

    for cp in stores:
        cp.wait()


def per_device(tokens, norm_gain, gate_trained, up_trained, down_trained):
    dma = pltpu.SemaphoreType.DMA
    g_t, u_t, d_o, m_t = pl.pallas_call(
        kernel,
        out_shape=(
            jax.ShapeDtypeStruct((OWN, D), BF),
            jax.ShapeDtypeStruct((OWN, D), BF),
            jax.ShapeDtypeStruct((OWN, D), BF),
            jax.ShapeDtypeStruct((32, TOK), BF),
        ),
        in_specs=[pl.BlockSpec(memory_space=pltpu.HBM)] * 5,
        out_specs=(pl.BlockSpec(memory_space=pltpu.HBM),) * 4,
        scratch_shapes=[
            pltpu.VMEM((TOK, D), BF),
            pltpu.VMEM((1, 32), F32),
            pltpu.VMEM((2, 32, 4 * GROUP), F32),
            pltpu.VMEM((OWN, 1024), F32),
            pltpu.VMEM((TPAD, D), BF),
            pltpu.VMEM((2, 8, OWN, 128), BF),
            pltpu.VMEM((NY, 4, OWN, 128), BF),
            pltpu.VMEM((NZ, OWN, 128), BF),
            pltpu.VMEM((NZ, OWN, 128), BF),
            pltpu.VMEM((2, OWN, D), BF),
            pltpu.VMEM((OWN, D), BF),
            pltpu.VMEM((8, OWN, 512), BF),
            pltpu.VMEM((8, OWN, 512), BF),
            pltpu.VMEM((8, OWN, TPAD), BF),
            pltpu.VMEM((NZ, 48, 128), BF),
            pltpu.VMEM((NZ, 48, 128), BF),
            pltpu.VMEM((32, TOK), BF),
            dma((5,)),
            dma((4,)),
            dma((16,)),
            dma((NY, 4)),
            dma((NZ,)),
            dma((NZ,)),
            dma((NY,)),
            dma((2, 2)),
            dma((NY,)),
            dma((NY,)),
            dma((8,)),
            dma((8,)),
            dma((8,)),
            dma((8,)),
            dma((NZ,)),
            dma((NZ,)),
        ],
        compiler_params=pltpu.CompilerParams(
            collective_id=0, has_side_effects=True, vmem_limit_bytes=48 * 1024 * 1024
        ),
        name="handoff",
    )(tokens, norm_gain.reshape(1, 32), gate_trained, up_trained, down_trained)
    return jnp.transpose(g_t), jnp.transpose(u_t), d_o, jnp.transpose(m_t)


def solution(mesh):
    split = Mesh(mesh.devices.reshape(NZ, NX, NC, NY), ("z", "x", "c", "y"))
    fs = ("z", "x", "c")
    in_specs = (P("y", None), P(fs), P(fs, "y"), P(fs, "y"), P(fs, "y"))
    out_specs = (P(None, fs), P(None, fs), P(fs, None), P("y", fs))
    return jax.shard_map(per_device, mesh=split, in_specs=in_specs, out_specs=out_specs, check_vma=False)
```

```python
import jax
import jax.numpy as jnp
from jax import lax
from jax.experimental import pallas as pl
from jax.experimental.pallas import tpu as pltpu
from jax.sharding import Mesh
from jax.sharding import PartitionSpec as P

LIMIT = 62000000
MESH = pl.DeviceIdType.MESH
BF = jnp.bfloat16
F32 = jnp.float32

NZ, NX, NC, NY = 16, 4, 2, 4
D, OWN, TOK, TPAD = 4096, 88, 192, 256
GROUP = 704


def lane_blocks_swapped(tiles):
    lane = lax.broadcasted_iota(jnp.int32, tiles[0].shape, 1) // 32
    outs = []
    for k in range(4):
        acc = None
        for t in range(4):
            shift = (32 * (t - k)) % 128
            moved = tiles[t] if shift == 0 else pltpu.roll(tiles[t], shift, 1)
            acc = moved if acc is None else jnp.where(lane == t, moved, acc)
        outs.append(acc)
    return outs


def kernel(
    tok, gain, gate, up, down, g_out, u_out, d_out, m_out,
    tok_v, gain_v, gu_v, down_v, normed, s_buf, ra, sb, rb, w, dn, db, d2, h, sr, rr, m_v,
    in_sem, out_sem,
    a_send, a_recv, b_send, b_recv, c_send, c_recv, d_send, d_recv, e_send, e_recv, h_send, h_recv, r_send, r_recv,
):
    z, x, c, y = (lax.axis_index(n) for n in ("z", "x", "c", "y"))
    xc = x * 2 + c
    loads = [
        pltpu.make_async_copy(gate, gu_v.at[0], in_sem.at[0]),
        pltpu.make_async_copy(up, gu_v.at[1], in_sem.at[1]),
        pltpu.make_async_copy(gain, gain_v, in_sem.at[2]),
        pltpu.make_async_copy(down, down_v, in_sem.at[3]),
        pltpu.make_async_copy(tok, tok_v, in_sem.at[4]),
    ]
    for cp in loads:
        cp.start()
    barrier = pltpu.get_barrier_semaphore()
    here = xc * 4 + y

    def greet_plane(n, _):
        other = lax.rem(here + n, 32)
        pl.semaphore_signal(
            barrier, inc=1, device_id=(z, other // 8, lax.rem(other // 4, 2), lax.rem(other, 4)), device_id_type=MESH
        )
        return 0

    def greet_line(n, _):
        pl.semaphore_signal(barrier, inc=1, device_id=(lax.rem(z + n, NZ), x, c, y), device_id_type=MESH)
        return 0

    lax.fori_loop(1, NZ, greet_line, 0)
    lax.fori_loop(1, 32, greet_plane, 0)

    loads[2].wait()
    gains = jnp.concatenate([gain_v[...]] * 4, axis=1)
    for g in range(2):
        loads[g].wait()
        stacked = jnp.concatenate([gu_v[g, :, GROUP * q : GROUP * (q + 1)] for q in range(4)], axis=0)
        turned = (jnp.transpose(stacked) * gains).astype(BF)
        for k in range(8):
            s_buf[g, k] = turned[OWN * k : OWN * (k + 1)]
    loads[3].wait()
    down_bf = down_v[...].astype(BF)
    dn[:, pl.ds(pl.multiple_of(1024 * y, 1024), 1024)] = down_bf

    pl.semaphore_wait(barrier, 46)

    half = x // 2
    sub = lax.rem(x, 2) * 2 + c

    def a_copy(n):
        to_x, to_y = lax.rem(x + n // 4, NX), lax.rem(y + n, NY)
        return pltpu.make_async_remote_copy(
            src_ref=s_buf.at[lax.rem(to_y, 2), to_x * 2 + to_y // 2],
            dst_ref=ra.at[y, sub],
            send_sem=a_send.at[n],
            recv_sem=a_recv.at[y, sub],
            device_id=(z, to_x, half, to_y),
            device_id_type=MESH,
        )

    def a_start(n, _):
        a_copy(n).start()
        return 0

    @pl.when(half != c)
    def _():
        a_copy(0).start()

    @pl.when(half == c)
    def _():
        ra[y, sub] = s_buf[lax.rem(y, 2), x * 2 + y // 2]

    lax.fori_loop(1, 16, a_start, 0)

    def d_copy(n):
        at = dn.at[:, pl.ds(pl.multiple_of(1024 * y, 1024), 1024)]
        return pltpu.make_async_remote_copy(
            src_ref=at, dst_ref=at, send_sem=d_send.at[n], recv_sem=d_recv.at[y],
            device_id=(z, x, c, lax.rem(y + n, NY)), device_id_type=MESH,
        )

    for n in (1, 3, 2):
        d_copy(n).start()

    loads[4].wait()

    def norm_rows(n, _):
        rows = pl.ds(pl.multiple_of(n * 16, 16), 16)
        t = tok_v[rows, :].astype(F32)
        normed[rows, :] = (t * lax.rsqrt(jnp.mean(t * t, axis=-1, keepdims=True) + 1e-06)).astype(BF)
        return 0

    lax.fori_loop(0, TOK // 16, norm_rows, 0)
    normed[TOK:, :] = jnp.zeros((TPAD - TOK, D), BF)

    def a_arrived(ys, s):
        @pl.when(jnp.logical_or(half != c, jnp.logical_or(ys != y, s != sub)))
        def _():
            pltpu.make_async_remote_copy(
                src_ref=ra.at[ys, s], dst_ref=ra.at[ys, s], send_sem=a_send.at[0], recv_sem=a_recv.at[ys, s],
                device_id=(z, x, 1 - c, y), device_id_type=MESH,
            ).wait_recv()

    def regroup(ys, _):
        for s in range(4):
            a_arrived(ys, s)
        outs = lane_blocks_swapped([ra[ys, s].astype(F32) for s in range(4)])
        for q in range(4):
            sb[ys * 4 + q] = outs[q].astype(BF)
        return 0

    lax.fori_loop(0, NY, regroup, 0)

    def near_first(i):
        return jnp.where(lax.rem(i, 2) == 1, (i + 1) // 2, NZ - i // 2)

    def b_copy(i):
        to_z = lax.rem(z + near_first(i), NZ)
        return pltpu.make_async_remote_copy(
            src_ref=sb.at[to_z], dst_ref=rb.at[z], send_sem=b_send.at[i], recv_sem=b_recv.at[z],
            device_id=(to_z, x, c, y), device_id_type=MESH,
        )

    def b_start(i, _):
        b_copy(i).start()
        return 0

    lax.fori_loop(1, NZ, b_start, 0)
    rb[z] = sb[z]

    own_c, own_g = y // 2, lax.rem(y, 2)

    def w_lanes(zs):
        return pl.ds(pl.multiple_of(256 * zs + 128 * c, 128), 128)

    def c_copy(zs, n):
        return pltpu.make_async_remote_copy(
            src_ref=rb.at[zs], dst_ref=w.at[own_g, :, w_lanes(zs)], send_sem=c_send.at[n], recv_sem=c_recv.at[own_g, c],
            device_id=(z, x, own_c, lax.rem(y + n, NY)), device_id_type=MESH,
        )

    def c_spread(zs):
        for n in (1, 3, 2):
            c_copy(zs, n).start()

        @pl.when(own_c != c)
        def _():
            c_copy(zs, 0).start()

        @pl.when(own_c == c)
        def _():
            w[own_g, :, w_lanes(zs)] = rb[zs]

    c_spread(z)

    def c_step(i, _):
        zs = lax.rem(z + NZ - near_first(i), NZ)
        pltpu.make_async_remote_copy(
            src_ref=rb.at[zs], dst_ref=rb.at[zs], send_sem=b_send.at[0], recv_sem=b_recv.at[zs],
            device_id=(lax.rem(z + 1, NZ), x, c, y), device_id_type=MESH,
        ).wait_recv()
        c_spread(zs)
        return 0

    lax.fori_loop(1, 8, c_step, 0)

    for n in (1, 2, 3):
        ys = lax.rem(y + NY - n, NY)
        at = dn.at[:, pl.ds(pl.multiple_of(1024 * ys, 1024), 1024)]
        pltpu.make_async_remote_copy(
            src_ref=at, dst_ref=at, send_sem=d_send.at[0], recv_sem=d_recv.at[ys],
            device_id=(z, x, 1 - c, y), device_id_type=MESH,
        ).wait_recv()
    d_store = pltpu.make_async_copy(dn, d_out, out_sem.at[2])
    d_store.start()

    def by_column(n, _):
        ys, hi = n // 2, lax.rem(n, 2)
        tiles = [
            dn[:, pl.ds(pl.multiple_of(1024 * ys + 256 * q + 128 * hi, 128), 128)].astype(F32) for q in range(4)
        ]
        outs = lane_blocks_swapped(tiles)
        for k in range(4):
            db[hi * 4 + k, :, pl.ds(pl.multiple_of(128 * ys, 128), 128)] = outs[k].astype(BF)
        return 0

    lax.fori_loop(0, 8, by_column, 0)

    def e_copy(n):
        to = lax.rem(xc + n, 8)
        return pltpu.make_async_remote_copy(
            src_ref=db.at[to], dst_ref=d2.at[xc], send_sem=e_send.at[n], recv_sem=e_recv.at[xc],
            device_id=(z, to // 2, lax.rem(to, 2), y), device_id_type=MESH,
        )

    def e_start(n, _):
        e_copy(n).start()
        return 0

    lax.fori_loop(1, 8, e_start, 0)
    d2[xc] = db[xc]

    lax.fori_loop(8, NZ, c_step, 0)

    stores = [d_store]
    for g in range(2):
        for k in range(2):
            @pl.when(jnp.logical_or(y != 2 * c + g, c != k))
            def _():
                pltpu.make_async_remote_copy(
                    src_ref=rb, dst_ref=rb, send_sem=c_send.at[0], recv_sem=c_recv.at[g, k],
                    device_id=(z, x, 1 - c, y), device_id_type=MESH,
                ).wait_recv()
        stores.append(pltpu.make_async_copy(w.at[g], (g_out, u_out)[g], out_sem.at[g]))
        stores[-1].start()

    acts = [
        lax.dot_general(w[g], normed[...], (((1,), (1,)), ((), ())), preferred_element_type=F32) for g in range(2)
    ]
    h[xc] = (acts[0] / (1.0 + jnp.exp(-acts[0])) * acts[1]).astype(BF)

    def h_copy(n):
        to = lax.rem(xc + n, 8)
        return pltpu.make_async_remote_copy(
            src_ref=h.at[xc], dst_ref=h.at[xc], send_sem=h_send.at[n], recv_sem=h_recv.at[xc],
            device_id=(z, to // 2, lax.rem(to, 2), y), device_id_type=MESH,
        )

    def h_start(n, _):
        h_copy(n).start()
        return 0

    lax.fori_loop(1, 8, h_start, 0)

    def plane_arrived(n, _):
        fr = lax.rem(xc + 8 - n, 8)
        pltpu.make_async_remote_copy(
            src_ref=d2.at[fr], dst_ref=d2.at[fr], send_sem=e_send.at[0], recv_sem=e_recv.at[fr],
            device_id=(z, x, 1 - c, y), device_id_type=MESH,
        ).wait_recv()
        pltpu.make_async_remote_copy(
            src_ref=h.at[fr], dst_ref=h.at[fr], send_sem=h_send.at[0], recv_sem=h_recv.at[fr],
            device_id=(z, x, 1 - c, y), device_id_type=MESH,
        ).wait_recv()
        return 0

    lax.fori_loop(1, 8, plane_arrived, 0)
    part = lax.dot_general(
        d2[...].reshape(8 * OWN, 512), h[...].reshape(8 * OWN, TPAD), (((0,), (0,)), ((), ())),
        preferred_element_type=F32,
    )
    lane = lax.broadcasted_iota(jnp.int32, (16, 128), 1)
    for q in range(NZ):
        block = part[32 * q : 32 * (q + 1)]
        tail = block[:, 128:]
        sr[q, :32] = block[:, :128].astype(BF)
        sr[q, 32:] = jnp.where(lane < 64, tail[:16], pltpu.roll(tail[16:], 64, 1)).astype(BF)

    def r_copy(i):
        to_z = lax.rem(z + near_first(i), NZ)
        return pltpu.make_async_remote_copy(
            src_ref=sr.at[to_z], dst_ref=rr.at[z], send_sem=r_send.at[i], recv_sem=r_recv.at[z],
            device_id=(to_z, x, c, y), device_id_type=MESH,
        )

    def r_start(i, _):
        r_copy(NZ - i).start()
        return 0

    lax.fori_loop(1, NZ, r_start, 0)

    def r_arrived(i, total):
        zs = lax.rem(z + NZ - near_first(i), NZ)
        pltpu.make_async_remote_copy(
            src_ref=rr.at[zs], dst_ref=rr.at[zs], send_sem=r_send.at[0], recv_sem=r_recv.at[zs],
            device_id=(lax.rem(z + 1, NZ), x, c, y), device_id_type=MESH,
        ).wait_recv()
        return total + rr[zs].astype(F32)

    total = lax.fori_loop(1, NZ, r_arrived, sr[z].astype(F32))
    m_v[:, :128] = total[:32].astype(BF)
    m_v[:16, 128:] = total[32:, :64].astype(BF)
    m_v[16:, 128:] = pltpu.roll(total[32:], 64, 1)[:, :64].astype(BF)
    m_store = pltpu.make_async_copy(m_v, m_out, out_sem.at[3])
    m_store.start()
    stores.append(m_store)

    @pl.when(half != c)
    def _():
        a_copy(0).wait_send()

    def a_sent(n, _):
        a_copy(n).wait_send()
        return 0

    lax.fori_loop(1, 16, a_sent, 0)

    def line_sent(i, _):
        b_copy(i).wait_send()
        r_copy(i).wait_send()
        return 0

    lax.fori_loop(1, NZ, line_sent, 0)

    def plane_sent(n, _):
        e_copy(n).wait_send()
        h_copy(n).wait_send()
        return 0

    lax.fori_loop(1, 8, plane_sent, 0)

    def c_sent(n):
        pltpu.make_async_remote_copy(
            src_ref=rb, dst_ref=rb, send_sem=c_send.at[n], recv_sem=c_recv.at[0, 0],
            device_id=(z, x, 1 - c, y), device_id_type=MESH,
        ).wait_send()

    for n in (1, 2, 3):
        d_copy(n).wait_send()
        c_sent(n)

    @pl.when(own_c != c)
    def _():
        c_sent(0)

    for cp in stores:
        cp.wait()


def hand_over(g_t, u_t, d_o, m_t, g_out, u_out, d_out, m_out, sem):
    copies = [
        pltpu.make_async_copy(a, b, sem.at[n])
        for n, (a, b) in enumerate(((g_t, g_out), (u_t, u_out), (d_o, d_out), (m_t, m_out)))
    ]
    for cp in copies:
        cp.start()
    for cp in copies:
        cp.wait()


def per_device(tokens, norm_gain, gate_trained, up_trained, down_trained):
    dma = pltpu.SemaphoreType.DMA
    g_t, u_t, d_o, m_t = pl.pallas_call(
        kernel,
        out_shape=(
            pltpu.VMEM((OWN, D), BF),
            pltpu.VMEM((OWN, D), BF),
            pltpu.VMEM((OWN, D), BF),
            pltpu.VMEM((32, TOK), BF),
        ),
        in_specs=[pl.BlockSpec(memory_space=pltpu.HBM)] * 5,
        out_specs=(pl.BlockSpec(memory_space=pltpu.VMEM),) * 4,
        scratch_shapes=[
            pltpu.VMEM((TOK, D), BF),
            pltpu.VMEM((1, 32), F32),
            pltpu.VMEM((2, 32, 4 * GROUP), F32),
            pltpu.VMEM((OWN, 1024), F32),
            pltpu.VMEM((TPAD, D), BF),
            pltpu.VMEM((2, 8, OWN, 128), BF),
            pltpu.VMEM((NY, 4, OWN, 128), BF),
            pltpu.VMEM((NZ, OWN, 128), BF),
            pltpu.VMEM((NZ, OWN, 128), BF),
            pltpu.VMEM((2, OWN, D), BF),
            pltpu.VMEM((OWN, D), BF),
            pltpu.VMEM((8, OWN, 512), BF),
            pltpu.VMEM((8, OWN, 512), BF),
            pltpu.VMEM((8, OWN, TPAD), BF),
            pltpu.VMEM((NZ, 48, 128), BF),
            pltpu.VMEM((NZ, 48, 128), BF),
            pltpu.VMEM((32, TOK), BF),
            dma((5,)),
            dma((4,)),
            dma((16,)),
            dma((NY, 4)),
            dma((NZ,)),
            dma((NZ,)),
            dma((NY,)),
            dma((2, 2)),
            dma((NY,)),
            dma((NY,)),
            dma((8,)),
            dma((8,)),
            dma((8,)),
            dma((8,)),
            dma((NZ,)),
            dma((NZ,)),
        ],
        compiler_params=pltpu.CompilerParams(
            collective_id=0, has_side_effects=True, vmem_limit_bytes=LIMIT
        ),
        name="handoff",
    )(tokens, norm_gain.reshape(1, 32), gate_trained, up_trained, down_trained)
    g_t, u_t, d_o, m_t = pl.pallas_call(
        hand_over,
        out_shape=tuple(jax.ShapeDtypeStruct(a.shape, a.dtype) for a in (g_t, u_t, d_o, m_t)),
        in_specs=[pl.BlockSpec(memory_space=pltpu.VMEM)] * 4,
        out_specs=(pl.BlockSpec(memory_space=pltpu.HBM),) * 4,
        scratch_shapes=[pltpu.SemaphoreType.DMA((4,))],
        compiler_params=pltpu.CompilerParams(vmem_limit_bytes=8 * 1024 * 1024),
        name="hand_over",
    )(g_t, u_t, d_o, m_t)
    return jnp.transpose(g_t), jnp.transpose(u_t), d_o, jnp.transpose(m_t)


def solution(mesh):
    split = Mesh(mesh.devices.reshape(NZ, NX, NC, NY), ("z", "x", "c", "y"))
    fs = ("z", "x", "c")
    in_specs = (P("y", None), P(fs), P(fs, "y"), P(fs, "y"), P(fs, "y"))
    out_specs = (P(None, fs), P(None, fs), P(fs, None), P("y", fs))
    return jax.shard_map(per_device, mesh=split, in_specs=in_specs, out_specs=out_specs, check_vma=False)
```

```python
import jax
import jax.numpy as jnp
from jax import lax
from jax.experimental import pallas as pl
from jax.experimental.pallas import tpu as pltpu
from jax.sharding import Mesh
from jax.sharding import PartitionSpec as P

LIMIT = 62000000
MESH = pl.DeviceIdType.MESH
BF = jnp.bfloat16
F32 = jnp.float32

NZ, NX, NC, NY = 16, 4, 2, 4
D, OWN, TOK, TPAD = 4096, 88, 192, 256
GROUP = 704
FAR_FIRST = sorted(
    ((dx, dc, dy) for dx in range(NX) for dc in range(NC) for dy in range(NY) if dx or dc or dy),
    key=lambda d: -min(d[0], NX - d[0]) - min(d[2], NY - d[2]),
)
WITH_LINE = {FAR_FIRST[1]: (4, 12), FAR_FIRST[9]: (3, 13), FAR_FIRST[17]: (2, 14), FAR_FIRST[-1]: (1, 15)}
CHUNKS = ((0, 48), (48, 40))
SWAP = (9, 16)
D_PASS, D_USE = 8, 4


def lane_blocks_swapped(tiles):
    lane = lax.broadcasted_iota(jnp.int32, tiles[0].shape, 1) // 32
    outs = []
    for k in range(4):
        acc = None
        for t in range(4):
            shift = (32 * (t - k)) % 128
            moved = tiles[t] if shift == 0 else pltpu.roll(tiles[t], shift, 1)
            acc = moved if acc is None else jnp.where(lane == t, moved, acc)
        outs.append(acc)
    return outs


def kernel(
    tok, gain, gate, up, down, g_out, u_out, d_out, m_out,
    tok_v, gain_v, gu_v, down_v, normed, s_buf, ra, sb, rb, w0, w1, dn, db, d2, h, hb, sr, rr,
    line_sem, in_sem, out_sem,
    a_send, a_recv, b_send, b_recv, c_send, c_recv, d_send, d_recv, e_send, e_recv, h_send, h_recv, r_send, r_recv,
):
    z, x, c, y = (lax.axis_index(n) for n in ("z", "x", "c", "y"))
    xc = x * 2 + c
    w = (w0, w1)
    barrier = pltpu.get_barrier_semaphore()
    for dx, dc, dy in FAR_FIRST:
        pl.semaphore_signal(
            barrier, inc=1, device_id=(z, lax.rem(x + dx, NX), lax.rem(c + dc, NC), lax.rem(y + dy, NY)), device_id_type=MESH
        )
        if (dx, dc, dy) in WITH_LINE:
            for dz in WITH_LINE[dx, dc, dy]:
                pl.semaphore_signal(barrier, inc=1, device_id=(lax.rem(z + dz, NZ), x, c, y), device_id_type=MESH)

    loads = [
        pltpu.make_async_copy(gate, gu_v.at[0], in_sem.at[0]),
        pltpu.make_async_copy(up, gu_v.at[1], in_sem.at[1]),
        pltpu.make_async_copy(gain, gain_v, in_sem.at[2]),
        pltpu.make_async_copy(down, down_v, in_sem.at[3]),
        pltpu.make_async_copy(tok, tok_v, in_sem.at[4]),
    ]
    for cp in loads:
        cp.start()
    loads[2].wait()
    gains = jnp.concatenate([gain_v[...]] * 4, axis=1)
    for g in range(2):
        loads[g].wait()
        stacked = jnp.concatenate([gu_v[g, :, GROUP * q : GROUP * (q + 1)] for q in range(4)], axis=0)
        turned = (jnp.transpose(stacked) * gains).astype(BF)
        for k in range(8):
            s_buf[g, k] = turned[OWN * k : OWN * (k + 1)]
    loads[3].wait()
    down_bf = down_v[...].astype(BF)
    dn[:, pl.ds(pl.multiple_of(1024 * y, 1024), 1024)] = down_bf

    pl.semaphore_wait(barrier, 39)

    half = x // 2
    sub = lax.rem(x, 2) * 2 + c

    def rows(ch):
        return pl.ds(*CHUNKS[ch])

    def a_copy(n, ch):
        to_x, to_y = lax.rem(x + n // 4, NX), lax.rem(y + n, NY)
        return pltpu.make_async_remote_copy(
            src_ref=s_buf.at[lax.rem(to_y, 2), to_x * 2 + to_y // 2, rows(ch)],
            dst_ref=ra.at[y, sub, rows(ch)],
            send_sem=a_send.at[0],
            recv_sem=a_recv.at[ch, y],
            device_id=(z, to_x, half, to_y),
            device_id_type=MESH,
        )

    @pl.when(half == c)
    def _():
        ra[y, sub] = s_buf[lax.rem(y, 2), x * 2 + y // 2]

    for ch in range(2):
        for n in sorted(range(1, 16), key=lambda n: -min(n // 4, 4 - n // 4) - min(n % 4, 4 - n % 4)):
            a_copy(n, ch).start()

        @pl.when(half != c)
        def _():
            a_copy(0, ch).start()

    for way in (4, NZ - 4):
        pl.semaphore_signal(line_sem, inc=1, device_id=(lax.rem(z + way, NZ), x, c, y), device_id_type=MESH)

    loads[4].wait()

    def norm_rows(n, _):
        some = pl.ds(pl.multiple_of(n * 16, 16), 16)
        t = tok_v[some, :].astype(F32)
        normed[some, :] = (t * lax.rsqrt(jnp.mean(t * t, axis=-1, keepdims=True) + 1e-06)).astype(BF)
        return 0

    lax.fori_loop(0, TOK // 16, norm_rows, 0)

    def landed(ref, sem):
        pltpu.make_async_remote_copy(
            src_ref=ref, dst_ref=ref, send_sem=a_send.at[0], recv_sem=sem,
            device_id=(z, x, 1 - c, y), device_id_type=MESH,
        ).wait_recv()

    def has_left(ref, sem):
        pltpu.make_async_remote_copy(
            src_ref=ref, dst_ref=ref, send_sem=sem, recv_sem=b_recv.at[0, 0],
            device_id=(z, x, 1 - c, y), device_id_type=MESH,
        ).wait_send()

    def regroup(ys, ch):
        mine = jnp.logical_and(half == c, ys == y)

        @pl.when(mine)
        def _():
            landed(ra.at[ys, pl.ds(0, 3), rows(ch)], a_recv.at[ch, ys])

        @pl.when(jnp.logical_not(mine))
        def _():
            landed(ra.at[ys, :, rows(ch)], a_recv.at[ch, ys])

        outs = lane_blocks_swapped([ra[ys, s, rows(ch)].astype(F32) for s in range(4)])
        for q in range(4):
            sb[ys * 4 + q, rows(ch)] = outs[q].astype(BF)
        return 0

    def near_first(i):
        if isinstance(i, int):
            return (i + 1) // 2 if i % 2 else NZ - i // 2
        return jnp.where(lax.rem(i, 2) == 1, (i + 1) // 2, NZ - i // 2)

    def at_turn(i, ch):
        if isinstance(i, int):
            return near_first(i if i < SWAP[ch] else NZ - 1 + SWAP[ch] - i)
        return near_first(jnp.where(i < SWAP[ch], i, NZ - 1 + SWAP[ch] - i))

    def source_z(i, ch):
        return lax.rem(z + NZ - at_turn(i, ch), NZ)

    def b_copy(i, ch):
        to_z = lax.rem(z + at_turn(i, ch), NZ)
        return pltpu.make_async_remote_copy(
            src_ref=sb.at[to_z, rows(ch)], dst_ref=rb.at[z, rows(ch)], send_sem=b_send.at[0], recv_sem=b_recv.at[ch, z],
            device_id=(to_z, x, c, y), device_id_type=MESH,
        )

    own_c, own_g = y // 2, lax.rem(y, 2)

    def w_lanes(zs):
        return pl.ds(pl.multiple_of(256 * zs + 128 * c, 128), 128)

    def w_rows(ch):
        return pl.ds(pl.multiple_of(CHUNKS[ch][1] * own_g, 8), CHUNKS[ch][1])

    def c_copy(zs, n, ch):
        return pltpu.make_async_remote_copy(
            src_ref=rb.at[zs, rows(ch)], dst_ref=w[ch].at[w_rows(ch), w_lanes(zs)],
            send_sem=c_send.at[n], recv_sem=c_recv.at[ch, own_g, c],
            device_id=(z, x, own_c, lax.rem(y + n, NY)), device_id_type=MESH,
        )

    def c_spread(zs, ch):
        for n in (1, 3, 2):
            c_copy(zs, n, ch).start()

        @pl.when(own_c != c)
        def _():
            c_copy(zs, 0, ch).start()

        @pl.when(own_c == c)
        def _():
            w[ch][w_rows(ch), w_lanes(zs)] = rb[zs, rows(ch)]

    def d_copy(ys, start, width, way, at):
        lanes = dn.at[:, pl.ds(pl.multiple_of(1024 * ys + start, 512), width)]
        return pltpu.make_async_remote_copy(
            src_ref=lanes, dst_ref=lanes, send_sem=d_send.at[0], recv_sem=d_recv.at[at],
            device_id=(z, x, c, lax.rem(y + way, NY)), device_id_type=MESH,
        )

    before, after, across = lax.rem(y + 3, NY), lax.rem(y + 1, NY), lax.rem(y + 2, NY)
    d_copies = [
        d_copy(y, 0, 1024, 1, 0), d_copy(y, 0, 1024, 3, 1), d_copy(before, 512, 512, 1, 2), d_copy(after, 0, 512, 3, 3)
    ]

    def d_landed(ys, start, width, at):
        landed(dn.at[:, pl.ds(pl.multiple_of(1024 * ys + start, 512), width)], d_recv.at[at])

    for ch in range(2):
        lax.fori_loop(0, NY, lambda ys, _: regroup(ys, ch), 0)
        if ch == 0:
            pl.semaphore_wait(line_sem, 2)

        for i in range(1, NZ):
            b_copy(i, ch).start()
        rb[z, rows(ch)] = sb[z, rows(ch)]
        if ch == 0:
            d_copies[0].start()
            d_copies[1].start()

    def c_step(i, ch):
        zs = source_z(i, ch)
        landed(rb.at[zs, rows(ch)], b_recv.at[ch, zs])
        c_spread(zs, ch)
        return 0

    c_spread(z, 0)
    c_spread(z, 1)
    lax.fori_loop(1, D_PASS, lambda i, _: c_step(i, 0), 0)
    d_landed(before, 0, 1024, 0)
    d_copies[2].start()
    d_landed(after, 0, 1024, 1)
    d_copies[3].start()
    lax.fori_loop(D_PASS, NZ, lambda i, _: c_step(i, 0), 0)
    lax.fori_loop(1, D_USE, lambda i, _: c_step(i, 1), 0)

    d_landed(across, 512, 512, 2)
    d_landed(across, 0, 512, 3)
    d_store = pltpu.make_async_copy(dn, d_out, out_sem.at[4])

    def by_column(n, _):
        ys, hi = n // 2, lax.rem(n, 2)
        tiles = [
            dn[:, pl.ds(pl.multiple_of(1024 * ys + 256 * q + 128 * hi, 128), 128)].astype(F32) for q in range(4)
        ]
        outs = lane_blocks_swapped(tiles)
        for k in range(4):
            db[hi * 4 + k, :, pl.ds(pl.multiple_of(128 * ys, 128), 128)] = outs[k].astype(BF)
        return 0

    lax.fori_loop(0, 8, by_column, 0)

    def e_copy(n):
        to = lax.rem(xc + n, 8)
        return pltpu.make_async_remote_copy(
            src_ref=db.at[to], dst_ref=d2.at[xc], send_sem=e_send.at[0], recv_sem=e_recv.at[0],
            device_id=(z, to // 2, lax.rem(to, 2), y), device_id_type=MESH,
        )

    def e_start(n, _):
        e_copy(n).start()
        return 0

    lax.fori_loop(1, 8, e_start, 0)
    d2[xc] = db[xc]

    lax.fori_loop(D_USE, NZ, lambda i, _: c_step(i, 1), 0)

    stores = [d_store]

    def h_copy(n, ch, t):
        to = lax.rem(xc + n, 8)
        ref = (h.at[xc, rows(ch), pl.ds(0, 128)], hb.at[ch, xc])[t]
        return pltpu.make_async_remote_copy(
            src_ref=ref, dst_ref=ref, send_sem=h_send.at[t], recv_sem=h_recv.at[ch, t],
            device_id=(z, to // 2, lax.rem(to, 2), y), device_id_type=MESH,
        )

    for ch, (first, count) in enumerate(CHUNKS):
        for g in range(2):
            for k in range(2):
                @pl.when(jnp.logical_or(y != 2 * c + g, c != k))
                def _():
                    landed(rb.at[:, rows(ch)], c_recv.at[ch, g, k])

            stores.append(
                pltpu.make_async_copy(
                    w[ch].at[pl.ds(count * g, count), :], (g_out, u_out)[g].at[rows(ch), :], out_sem.at[2 * ch + g]
                )
            )

        acts = lax.dot_general(w[ch][...], normed[...], (((1,), (1,)), ((), ())), preferred_element_type=F32)
        hidden = acts[:count] / (1.0 + jnp.exp(-acts[:count])) * acts[count:]
        h[xc, first : first + count, :128] = hidden[:, :128].astype(BF)
        below = hidden[24:, 128:]
        if count < 48:
            below = jnp.concatenate([below, jnp.zeros((48 - count, 64), F32)], axis=0)
        hb[ch, xc] = jnp.concatenate([hidden[:24, 128:], below], axis=1).astype(BF)
        for t in range(2):
            for n in (4, 5, 3, 2, 6, 7, 1):
                h_copy(n, ch, t).start()

    for ch, (first, count) in enumerate(CHUNKS):
        landed(rb.at[pl.ds(0, 7), rows(ch)], h_recv.at[ch, 0])
        landed(hb.at[ch, pl.ds(0, 7)], h_recv.at[ch, 1])
        for n in range(8):
            packed = hb[ch, n].astype(F32)
            h[n, first : first + 24, 128:] = packed.astype(BF)
            h[n, first + 24 : first + count, 128:] = pltpu.roll(packed, 64, 1)[: count - 24].astype(BF)
    landed(d2.at[pl.ds(0, 7)], e_recv.at[0])
    part = lax.dot_general(
        d2[...].reshape(8 * OWN, 512), h[...].reshape(8 * OWN, TPAD), (((0,), (0,)), ((), ())),
        preferred_element_type=F32,
    )
    lane = lax.broadcasted_iota(jnp.int32, (16, 128), 1)
    for q in range(NZ):
        block = part[32 * q : 32 * (q + 1)]
        tail = block[:, 128:]
        sr[q, :32] = block[:, :128].astype(BF)
        sr[q, 32:] = jnp.where(lane < 64, tail[:16], pltpu.roll(tail[16:], 64, 1)).astype(BF)

    def r_copy(to_z):
        return pltpu.make_async_remote_copy(
            src_ref=sr.at[to_z], dst_ref=rr.at[z], send_sem=r_send.at[0], recv_sem=r_recv.at[0],
            device_id=(to_z, x, c, y), device_id_type=MESH,
        )

    for to_z in range(NZ):
        @pl.when(to_z != z)
        def _():
            r_copy(to_z).start()

    for cp in stores:
        cp.start()
    rr[z] = sr[z]
    landed(rr.at[pl.ds(0, NZ - 1)], r_recv.at[0])
    total = rr[0].astype(F32)
    for q in range(1, NZ):
        total += rr[q].astype(F32)
    m_out[:, :128] = total[:32].astype(BF)
    m_out[:16, 128:] = total[32:, :64].astype(BF)
    m_out[16:, 128:] = pltpu.roll(total[32:], 64, 1)[:, :64].astype(BF)

    @pl.when(half != c)
    def _():
        has_left(ra, a_send.at[0])

    @pl.when(half == c)
    def _():
        has_left(rb.at[pl.ds(0, NZ - 1)], a_send.at[0])

    has_left(rb.at[pl.ds(0, NZ - 1)], b_send.at[0])
    has_left(sr.at[pl.ds(0, NZ - 1)], r_send.at[0])
    has_left(db.at[pl.ds(0, 7)], e_send.at[0])
    has_left(rb.at[pl.ds(0, 7)], h_send.at[0])
    has_left(hb.at[:, pl.ds(0, 7)], h_send.at[1])
    has_left(dn.at[:, pl.ds(0, 3072)], d_send.at[0])
    for n in (1, 2, 3):
        has_left(rb, c_send.at[n])

    @pl.when(own_c != c)
    def _():
        has_left(rb, c_send.at[0])

    for cp in stores:
        cp.wait()


def hand_over(g_t, u_t, d_o, m_t, g_out, u_out, d_out, m_out, sem):
    copies = [pltpu.make_async_copy(m_t, m_out, sem.at[0])]
    for a, b in ((g_t, g_out), (u_t, u_out), (d_o, d_out)):
        for first, count in ((0, 48), (48, 40)):
            some = pl.ds(first, count)
            copies.append(pltpu.make_async_copy(a.at[some, :], b.at[some, :], sem.at[len(copies)]))
    for cp in copies:
        cp.start()
    for cp in copies:
        cp.wait()


def per_device(tokens, norm_gain, gate_trained, up_trained, down_trained):
    dma = pltpu.SemaphoreType.DMA
    g_t, u_t, d_o, m_t = pl.pallas_call(
        kernel,
        out_shape=(
            pltpu.VMEM((OWN, D), BF),
            pltpu.VMEM((OWN, D), BF),
            pltpu.VMEM((OWN, D), BF),
            pltpu.VMEM((32, TOK), BF),
        ),
        in_specs=[pl.BlockSpec(memory_space=pltpu.HBM)] * 5,
        out_specs=(pl.BlockSpec(memory_space=pltpu.VMEM),) * 4,
        scratch_shapes=[
            pltpu.VMEM((TOK, D), BF),
            pltpu.VMEM((1, 32), F32),
            pltpu.VMEM((2, 32, 4 * GROUP), F32),
            pltpu.VMEM((OWN, 1024), F32),
            pltpu.VMEM((TOK, D), BF),
            pltpu.VMEM((2, 8, OWN, 128), BF),
            pltpu.VMEM((NY, 4, OWN, 128), BF),
            pltpu.VMEM((NZ, OWN, 128), BF),
            pltpu.VMEM((NZ, OWN, 128), BF),
            pltpu.VMEM((2 * CHUNKS[0][1], D), BF),
            pltpu.VMEM((2 * CHUNKS[1][1], D), BF),
            pltpu.VMEM((OWN, D), BF),
            pltpu.VMEM((8, OWN, 512), BF),
            pltpu.VMEM((8, OWN, 512), BF),
            pltpu.VMEM((8, OWN, TPAD), BF),
            pltpu.VMEM((2, 8, 24, 128), BF),
            pltpu.VMEM((NZ, 48, 128), BF),
            pltpu.VMEM((NZ, 48, 128), BF),
            pltpu.SemaphoreType.REGULAR,
            dma((5,)),
            dma((5,)),
            dma((1,)),
            dma((2, NY)),
            dma((1,)),
            dma((2, NZ)),
            dma((4,)),
            dma((2, 2, 2)),
            dma((1,)),
            dma((4,)),
            dma((1,)),
            dma((1,)),
            dma((2,)),
            dma((2, 2)),
            dma((1,)),
            dma((1,)),
        ],
        compiler_params=pltpu.CompilerParams(
            collective_id=0, has_side_effects=True, vmem_limit_bytes=LIMIT
        ),
        name="handoff",
    )(tokens, norm_gain.reshape(1, 32), gate_trained, up_trained, down_trained)
    g_t, u_t, d_o, m_t = pl.pallas_call(
        hand_over,
        out_shape=tuple(jax.ShapeDtypeStruct(a.shape, a.dtype) for a in (g_t, u_t, d_o, m_t)),
        in_specs=[pl.BlockSpec(memory_space=pltpu.VMEM)] * 4,
        out_specs=(pl.BlockSpec(memory_space=pltpu.HBM),) * 4,
        scratch_shapes=[pltpu.SemaphoreType.DMA((7,))],
        compiler_params=pltpu.CompilerParams(vmem_limit_bytes=8 * 1024 * 1024),
        name="hand_over",
    )(g_t, u_t, d_o, m_t)
    return jnp.transpose(g_t), jnp.transpose(u_t), d_o, jnp.transpose(m_t)


def solution(mesh):
    split = Mesh(mesh.devices.reshape(NZ, NX, NC, NY), ("z", "x", "c", "y"))
    fs = ("z", "x", "c")
    in_specs = (P("y", None), P(fs), P(fs, "y"), P(fs, "y"), P(fs, "y"))
    out_specs = (P(None, fs), P(None, fs), P(fs, None), P("y", fs))
    return jax.shard_map(per_device, mesh=split, in_specs=in_specs, out_specs=out_specs, check_vma=False)
```
